32 devices in a mesh: sp: 16 (over z, y, x), tp: 2 (over core).
Axes of the slice: x: 2, y: 2, z: 4, core: 2. Of those that a mesh axis runs over, the one named last changes fastest.
Arguments:
- latent: bfloat16 [4096, 2048], P(('sp', 'tp')), may hold values from -6 to 6
- context: bfloat16 [512, 2048], P('sp'), may hold values from -6 to 6
- condition: float32 [2048], P('tp'), may hold values from -6 to 6
- context_condition: float32 [2048], P('tp'), may hold values from -6 to 6
- modulation_weight: bfloat16 [2048, 6144], P('tp', 'sp'), may hold values from -0.125 to 0.125
- query_first: bfloat16 [2048, 512], P(None, 'tp'), may hold values from -1 to 1
- query_second: bfloat16 [2048, 512], P(None, 'tp'), may hold values from -1 to 1
- key_first: bfloat16 [2048, 512], P(None, 'tp'), may hold values from -1 to 1
- key_second: bfloat16 [2048, 512], P(None, 'tp'), may hold values from -1 to 1
- value_weight: bfloat16 [2048, 1024], P(None, 'tp'), may hold values from -0.125 to 0.125
- lambda_head: float32 [8], P('tp'), may hold values from 0.3 to 0.8
- context_score_boost: float32 [8], P('tp'), may hold values from 1.5 to 3
- head_gain: float32 [128], replicated, may hold values from 0.1 to 1.9
- output_weight: bfloat16 [1024, 2048], P('tp'), may hold values from -0.1875 to 0.1875
Outputs:
- updated: bfloat16 [4096, 2048], P(('sp', 'tp'))
The draws below stay inside these ranges and needn't reach their ends.
All inputs are finite; a program needn't handle non-finite values.
Results may differ from the reference program's by a relative error of at most 0.0095.
Values may be sent and summed in bfloat16 or wider, within the bound.
No kernel may reach another device: no remote copies, remote signals or barrier semaphores. Data moves between devices by JAX's collectives and lax.ppermute only.
A program may use at most 64 MiB of HBM per device.

```python
import jax
import jax.numpy as jnp
from jax import lax

D = 2048
HEADS = 8
HEAD_DIM = 64
VALUE_DIM = 128
GRID_W = 64
CTX = 512
TOKENS = 4096


def drawn_weight(key, stream):
    jitter = jax.random.normal(jax.random.fold_in(key, stream), (D, HEADS * HEAD_DIM), jnp.float32)
    return jnp.clip(jitter, -6.0, 6.0) * D ** (-0.5)


def draw_latent(key, part):
    jitter = jax.random.normal(jax.random.fold_in(key, 21), (TOKENS, D), jnp.float32)
    result = jnp.clip(jitter, -6.0, 6.0)
    return result.astype(jnp.bfloat16)


def draw_query_first(key, part):
    result = drawn_weight(key, 31)
    return jnp.clip(result, -1.0, 1.0).astype(jnp.bfloat16)


def draw_key_first(key, part):
    result = drawn_weight(key, 32)
    return jnp.clip(result, -1.0, 1.0).astype(jnp.bfloat16)


def draw_query_second(key, part):
    result = drawn_weight(key, 33)
    return jnp.clip(result, -1.0, 1.0).astype(jnp.bfloat16)


def draw_key_second(key, part):
    result = drawn_weight(key, 34)
    return jnp.clip(result, -1.0, 1.0).astype(jnp.bfloat16)


def shard_levels(stream_key, extent, cuts, smallest, largest):
    def one(position, shards_of):
        draws = jax.random.uniform(jax.random.fold_in(jax.random.fold_in(stream_key, 6), position), (shards_of,), jnp.float32, smallest / len(cuts), largest / len(cuts))
        return jnp.repeat(jnp.exp(draws), extent[position] // shards_of).reshape((-1,) + (1,) * (len(extent) - position - 1))

    factor_of = one(*cuts[0])
    for cut in cuts[1:]:
        factor_of = factor_of * one(*cut)
    return factor_of


def gaussian(stream_key, dims, scale, limit, split=(), kind=jnp.bfloat16):
    loudness = shard_levels(stream_key, dims, split, -0.22, 0.18) if split else 1.0
    values = jax.random.normal(stream_key, dims, jnp.float32) * scale * loudness
    return jnp.minimum(jnp.maximum(values, -limit), limit).astype(kind)


def setup_inputs(seed: int = 0) -> dict:
    key_list = jax.random.split(jax.random.key(seed), 15)
    latent = draw_latent(jax.random.fold_in(key_list[14], 71), 0)
    context = gaussian(key_list[1], (CTX, D), 1.0, 6.0, ((0, 16),))
    condition = gaussian(key_list[2], (D,), 1.0, 6.0, ((0, 2),), jnp.float32)
    context_condition = gaussian(key_list[3], (D,), 1.0, 6.0, ((0, 2),), jnp.float32)
    modulation_weight = gaussian(key_list[4], (D, 3 * D), D ** -0.5, 0.125, ((0, 2), (1, 16)))
    query_first = draw_query_first(jax.random.fold_in(key_list[14], 71), 0)
    query_second = draw_query_second(jax.random.fold_in(key_list[14], 71), 0)
    key_first = draw_key_first(jax.random.fold_in(key_list[14], 71), 0)
    key_second = draw_key_second(jax.random.fold_in(key_list[14], 71), 0)
    value_weight = gaussian(key_list[9], (D, HEADS * VALUE_DIM), D ** -0.5, 0.125, ((1, 2),))
    lambda_head = jnp.clip(0.3 + 0.5 * jax.random.uniform(key_list[10], (HEADS,), jnp.float32) ** shard_levels(key_list[10], (HEADS,), ((0, 2),), -0.2, 0.2), 0.3, 0.8)
    context_score_boost = jnp.clip(1.5 + 1.5 * jax.random.uniform(key_list[11], (HEADS,), jnp.float32) ** shard_levels(key_list[11], (HEADS,), ((0, 2),), -0.2, 0.2), 1.5, 3.0)
    head_gain = jnp.clip(1.0 + 0.18 * jax.random.normal(key_list[12], (VALUE_DIM,), jnp.float32), 0.1, 1.9)
    output_weight = gaussian(key_list[13], (HEADS * VALUE_DIM, D), (HEADS * VALUE_DIM) ** -0.5, 0.1875, ((0, 2),))
    return {"latent": latent, "context": context, "condition": condition, "context_condition": context_condition, "modulation_weight": modulation_weight, "query_first": query_first, "query_second": query_second, "key_first": key_first, "key_second": key_second, "value_weight": value_weight, "lambda_head": lambda_head, "context_score_boost": context_score_boost, "head_gain": head_gain, "output_weight": output_weight}


EPSILON = 1e-06
THETA = 10000.0

def norm_rows(rows):
    values = rows.astype(jnp.float32)
    return values * lax.rsqrt(lax.optimization_barrier(jnp.mean(values * values, axis=-1, keepdims=True)) + EPSILON)

def rotate_pairs(values, positions):
    half = values.shape[-1] // 2
    quarter = half // 2
    reciprocal_norm = THETA ** (-jnp.arange(quarter, dtype=jnp.float32) / quarter)

    def turn(part, where):
        angle = where.astype(jnp.float32)[:, None] * reciprocal_norm[None, :]
        cosine_table = jnp.concatenate([jnp.cos(angle)] * 2, -1)[:, None, :]
        sine = jnp.concatenate([jnp.sin(angle)] * 2, -1)[:, None, :]
        flipped = jnp.concatenate([-part[..., quarter:], part[..., :quarter]], -1)
        return part * cosine_table + flipped * sine
    grid_row = positions // GRID_W
    grid_col = positions % GRID_W
    return jnp.concatenate([turn(values[..., :half], grid_row), turn(values[..., half:], grid_col)], -1)

def project(rows, weight):
    return jnp.dot(rows, weight, preferred_element_type=jnp.float32).reshape(rows.shape[0], HEADS, -1)

def reference(latent, context, condition, context_condition, modulation_weight, query_first, query_second, key_first, key_second, value_weight, lambda_head, context_score_boost, head_gain, output_weight):
    signal = jax.nn.silu(jnp.stack([condition, context_condition])).astype(jnp.bfloat16)
    modulation = jnp.dot(signal, modulation_weight, preferred_element_type=jnp.float32)
    shift = modulation[:, :D]
    scale = modulation[:, D:2 * D]
    gate = modulation[:, 2 * D:]
    h_latent = (norm_rows(latent) * (1.0 + scale[0]) + shift[0]).astype(jnp.bfloat16)
    h_context = (norm_rows(context) * (1.0 + scale[1]) + shift[1]).astype(jnp.bfloat16)
    positions = jnp.arange(TOKENS, dtype=jnp.int32)
    queries_one = rotate_pairs(project(h_latent, query_first), positions).astype(jnp.bfloat16)
    queries_two = rotate_pairs(project(h_latent, query_second), positions).astype(jnp.bfloat16)
    latent_one = rotate_pairs(project(h_latent, key_first), positions).astype(jnp.bfloat16)
    latent_two = rotate_pairs(project(h_latent, key_second), positions).astype(jnp.bfloat16)
    latent_values = project(h_latent, value_weight).astype(jnp.bfloat16)
    context_one = project(h_context, key_first).astype(jnp.bfloat16)
    context_two = project(h_context, key_second).astype(jnp.bfloat16)
    context_values = project(h_context, value_weight).astype(jnp.bfloat16)
    keys_one = jnp.concatenate([context_one, latent_one], 0).astype(jnp.float32)
    keys_two = jnp.concatenate([context_two, latent_two], 0).astype(jnp.float32)
    values_all = jnp.concatenate([context_values, latent_values], 0).astype(jnp.float32)
    lift = jnp.concatenate([jnp.broadcast_to(context_score_boost[:, None], (HEADS, CTX)), jnp.zeros((HEADS, TOKENS), jnp.float32)], 1)[:, None, :]
    block = 256 if TOKENS % 256 == 0 else TOKENS
    count = TOKENS // block

    def attend(pair):
        query_one, query_two = pair
        outcomes = []
        for query, keys in ((query_one, keys_one), (query_two, keys_two)):
            scores = jnp.einsum('qhd,khd->hqk', query.astype(jnp.float32), keys) * HEAD_DIM ** (-0.5) + lift
            highest = lax.optimization_barrier(jnp.max(scores, axis=-1, keepdims=True))
            exp_weights = jnp.exp(scores - highest)
            totals = lax.optimization_barrier(jnp.sum(exp_weights, axis=-1))
            rounded = lax.optimization_barrier(exp_weights.astype(jnp.bfloat16))
            weighted = jnp.einsum('hqk,khe->qhe', rounded.astype(jnp.float32), values_all)
            outcomes.append(weighted / jnp.transpose(totals)[:, :, None])
        return outcomes[0] - lambda_head[None, :, None] * outcomes[1]
    blocks = (queries_one.reshape(count, block, HEADS, HEAD_DIM), queries_two.reshape(count, block, HEADS, HEAD_DIM))
    mixed = lax.map(attend, blocks).reshape(TOKENS, HEADS, VALUE_DIM)
    normed = mixed * lax.rsqrt(lax.optimization_barrier(jnp.mean(mixed * mixed, axis=-1, keepdims=True)) + EPSILON) * head_gain
    heads_out = normed.astype(jnp.bfloat16).reshape(TOKENS, HEADS * VALUE_DIM)
    branch = jnp.dot(heads_out, output_weight, preferred_element_type=jnp.float32)
    return (latent.astype(jnp.float32) + gate[0] * branch).astype(jnp.bfloat16)
```

```python
import functools
import math

import jax
import jax.numpy as jnp
from jax import lax
from jax.experimental import pallas as pl
from jax.experimental.pallas import tpu as pltpu
from jax.sharding import Mesh, PartitionSpec as P

HEAD_DIM = 64
VALUE_DIM = 128
GRID_W = 64
EPSILON = 1e-06
THETA = 10000.0
SP = ("g", "s")
ALL = ("g", "s", "tp")


def norm_rows(rows):
    values = rows.astype(jnp.float32)
    return values * lax.rsqrt(jnp.mean(values * values, axis=-1, keepdims=True) + EPSILON)


def shifts_over(array, axis, size):
    out = [array]
    for k in range(1, size):
        out.append(lax.ppermute(array, axis, [(i, (i + k) % size) for i in range(size)]))
    return out


def in_order(parts, index):
    size = len(parts)
    if size == 1:
        return jnp.stack(parts)
    if size == 2:
        a, b = parts
        first = index == 0
        return jnp.stack([jnp.where(first, a, b), jnp.where(first, b, a)])
    stacked = jnp.stack(parts)
    return jnp.take(stacked, (index - jnp.arange(size)) % size, axis=0)


def rope_tables(positions, extra):
    quarter = HEAD_DIM // 4
    reciprocal = THETA ** (-jnp.arange(quarter, dtype=jnp.float32) / quarter)
    row = (positions // GRID_W).astype(jnp.float32)[:, None] * reciprocal[None, :]
    col = (positions % GRID_W).astype(jnp.float32)[:, None] * reciprocal[None, :]
    angle = jnp.concatenate([row, row, col, col] * 2, -1)
    sign = jnp.where((jnp.arange(2 * HEAD_DIM) // quarter) % 2 == 0, -1.0, 1.0)
    cosine = jnp.cos(angle)
    sine = jnp.sin(angle) * sign[None, :]
    width = angle.shape[1]
    cosine = jnp.concatenate([cosine, jnp.ones((extra, width), jnp.float32)], 0)
    sine = jnp.concatenate([sine, jnp.zeros((extra, width), jnp.float32)], 0)
    return cosine, sine


def attention_kernel(first, last, scal, gain, q_ref, kv_ref, ctx_ref, *refs):
    refs = list(refs)
    vaug, vctx = refs[-2:]
    refs = refs[:-2]
    if not first:
        old, refs = refs[:4], refs[4:]
    out = refs

    @pl.when(pl.program_id(0) == 0)
    def _():
        vaug[:, :VALUE_DIM] = kv_ref[:, 2 * HEAD_DIM :]
        vaug[:, VALUE_DIM:] = jnp.ones((vaug.shape[0], VALUE_DIM), vaug.dtype)
        vctx[:, :VALUE_DIM] = ctx_ref[:, 2 * HEAD_DIM :]
        vctx[:, VALUE_DIM:] = jnp.ones((vctx.shape[0], VALUE_DIM), vctx.dtype)

    q = q_ref[...]
    lane = lax.broadcasted_iota(jnp.int32, q.shape, 1)
    boost = scal[0]
    dims = (((1,), (1,)), ((), ()))
    results = []
    for m in range(2):
        query = jnp.where((lane < HEAD_DIM) == (m == 0), q, jnp.zeros_like(q))
        s_lat = lax.dot_general(
            query, kv_ref[:, : 2 * HEAD_DIM], dims, preferred_element_type=jnp.float32
        )
        s_ctx = lax.dot_general(
            query, ctx_ref[:, : 2 * HEAD_DIM], dims, preferred_element_type=jnp.float32
        ) + boost
        peak = jnp.maximum(
            jnp.max(s_lat, axis=-1, keepdims=True), jnp.max(s_ctx, axis=-1, keepdims=True)
        )
        if not first:
            before = old[2 + m][...][:, :1]
            peak = jnp.maximum(peak, before)
        p_lat = jnp.exp2(s_lat - peak).astype(jnp.bfloat16)
        p_ctx = jnp.exp2(s_ctx - peak).astype(jnp.bfloat16)
        acc = jnp.dot(p_lat, vaug[...], preferred_element_type=jnp.float32) + jnp.dot(
            p_ctx, vctx[...], preferred_element_type=jnp.float32
        )
        if not first:
            acc = acc + old[m][...] * jnp.exp2(before - peak)
        if last:
            results.append(acc[:, :VALUE_DIM] / acc[:, VALUE_DIM:])
        else:
            out[m][...] = acc
            out[2 + m][...] = jnp.broadcast_to(peak, (q.shape[0], 128))
    if last:
        mixed = results[0] - scal[1] * results[1]
        scale = lax.rsqrt(jnp.mean(mixed * mixed, axis=-1, keepdims=True) + EPSILON)
        out[0][...] = (mixed * scale * gain[...]).astype(out[0].dtype)


def attend(scal, gain, queries, kv, ctx, state, last):
    count = queries.shape[0]
    tile = math.gcd(count, 256)
    rows = lambda width: pl.BlockSpec((tile, width), lambda i: (i, 0))
    whole = lambda a: pl.BlockSpec(a.shape, lambda i: (0, 0))
    state_shapes = [jax.ShapeDtypeStruct((count, w), jnp.float32) for w in (256, 256, 128, 128)]
    state_specs = [rows(s.shape[1]) for s in state_shapes]
    first = state is None
    if last:
        shapes = jax.ShapeDtypeStruct((count, VALUE_DIM), jnp.bfloat16)
        specs = rows(VALUE_DIM)
    else:
        shapes, specs = state_shapes, state_specs
    return pl.pallas_call(
        functools.partial(attention_kernel, first, last),
        grid=(count // tile,),
        in_specs=[pl.BlockSpec(memory_space=pltpu.SMEM), whole(gain), rows(128), whole(kv), whole(ctx)]
        + ([] if first else state_specs),
        out_specs=specs,
        out_shape=shapes,
        scratch_shapes=[
            pltpu.VMEM((kv.shape[0], 2 * VALUE_DIM), jnp.bfloat16),
            pltpu.VMEM((ctx.shape[0], 2 * VALUE_DIM), jnp.bfloat16),
        ],
        compiler_params=pltpu.CompilerParams(
            dimension_semantics=("arbitrary",), vmem_limit_bytes=56 * 2**20
        ),
        name="attend_last" if last else "attend_first" if first else "attend_next",
    )(scal, gain, queries, kv, ctx, *([] if first else state))


def body(
    latent,
    context,
    condition,
    context_condition,
    modulation_weight,
    query_first,
    query_second,
    key_first,
    key_second,
    value_weight,
    lambda_head,
    context_score_boost,
    head_gain,
    output_weight,
):
    width = latent.shape[1]
    tp = lax.axis_size("tp")
    sp = lax.axis_size(SP)
    groups = lax.axis_size("g")
    t = lax.axis_index("tp")
    head = lax.axis_index("s")
    heads_dev = value_weight.shape[1] // VALUE_DIM
    heads = heads_dev * tp

    signal = jax.nn.silu(jnp.stack([condition, context_condition])).astype(jnp.bfloat16)
    partial_mod = jnp.dot(signal, modulation_weight, preferred_element_type=jnp.float32)
    columns = partial_mod.shape[1]
    message = jnp.concatenate([partial_mod.reshape(-1), lambda_head, context_score_boost])
    pad = -message.shape[0] % 128
    message = jnp.pad(message, (0, pad))
    received = lax.all_to_all(
        jnp.broadcast_to(message[None], (sp * tp, message.shape[0])), ALL, 0, 0
    ).reshape(sp, tp, -1)
    modulation = jnp.sum(received[:, :, : 2 * columns], axis=1).reshape(sp, 2, columns)
    modulation = jnp.transpose(modulation, (1, 0, 2)).reshape(2, sp * columns)
    lambdas = received[0, :, 2 * columns : 2 * columns + heads_dev].reshape(heads)
    boosts = received[0, :, 2 * columns + heads_dev : 2 * columns + 2 * heads_dev].reshape(heads)
    scal = jnp.stack([boosts[head] * math.log2(math.e), lambdas[head]])
    shift = modulation[:, :width]
    scale = modulation[:, width : 2 * width]
    gate = modulation[0, 2 * width :]

    packs = [
        shifts_over(w, "tp", tp)
        for w in (query_first, query_second, key_first, key_second, value_weight)
    ]
    out_weights = shifts_over(output_weight, "tp", tp)
    rows = latent.shape[0]
    rows_ctx = context.shape[0] // tp
    ctx_own = lax.dynamic_slice_in_dim(context, t * rows_ctx, rows_ctx, 0)
    h_latent = (norm_rows(latent) * (1.0 + scale[0]) + shift[0]).astype(jnp.bfloat16)
    h_context = (norm_rows(ctx_own) * (1.0 + scale[1]) + shift[1]).astype(jnp.bfloat16)
    h = jnp.concatenate([h_latent, h_context], 0)
    offset = (lax.axis_index(SP) * tp + t) * rows
    cosine, sine = rope_tables(offset + jnp.arange(rows, dtype=jnp.int32), rows_ctx)
    quarter = HEAD_DIM // 4

    def project(weight, turn, factor=None):
        product = jnp.dot(h, weight, preferred_element_type=jnp.float32)
        if turn:
            reps = product.shape[1] // HEAD_DIM
            table_c = jnp.tile(cosine[:, :HEAD_DIM], (1, reps))
            table_s = jnp.tile(sine[:, :HEAD_DIM], (1, reps))
            lower = (jnp.arange(product.shape[1]) // quarter) % 2 == 0
            flipped = jnp.where(
                lower[None, :], jnp.roll(product, -quarter, 1), jnp.roll(product, quarter, 1)
            )
            product = product * table_c + flipped * table_s
            if factor is not None:
                product = product * factor
        return product.astype(jnp.bfloat16).reshape(h.shape[0], heads_dev, -1)

    factor = HEAD_DIM ** (-0.5) * math.log2(math.e)
    q_parts, kv_parts = [], []
    for k in range(tp):
        q1, q2, k1, k2 = (
            project(packs[n][k], True, factor if n < 2 else None) for n in range(4)
        )
        v = project(packs[4][k], False)
        q_parts.append(jnp.transpose(jnp.concatenate([q1, q2], -1)[:rows], (1, 0, 2)))
        kv_parts.append(jnp.transpose(jnp.concatenate([k1, k2, v], -1), (1, 0, 2)))
    q_all = in_order(q_parts, t).reshape(heads, rows, 2 * HEAD_DIM)
    kv_all = in_order(kv_parts, t).reshape(heads, rows + rows_ctx, 2 * HEAD_DIM + VALUE_DIM)

    queries = lax.all_to_all(q_all, "s", 0, 0).reshape(heads * rows, 2 * HEAD_DIM)
    kv_sent = jnp.broadcast_to(kv_all[None], (groups,) + kv_all.shape)
    kv_sent = kv_sent.reshape((sp,) + kv_all.shape[1:])
    kv = lax.all_to_all(kv_sent, SP, 0, 0)
    kv_each = shifts_over(kv, "tp", tp)
    gain = head_gain[None, :]
    state = None
    for k, part in enumerate(kv_each):
        lat = part[:, :rows].reshape(sp * rows, -1)
        ctx = part[:, rows:].reshape(sp * rows_ctx, -1)
        state = attend(scal, gain, queries, lat, ctx, state, k == tp - 1)
    heads_out = lax.all_to_all(state.reshape(heads, rows, VALUE_DIM), "s", 0, 0)

    grouped = heads_out.reshape(tp, heads_dev, rows, VALUE_DIM)
    branch = 0.0
    for k in range(tp):
        own = lax.dynamic_index_in_dim(grouped, (t - k) % tp, 0, keepdims=False)
        own = jnp.transpose(own, (1, 0, 2)).reshape(rows, heads_dev * VALUE_DIM)
        branch = branch + jnp.dot(own, out_weights[k], preferred_element_type=jnp.float32)
    return (latent.astype(jnp.float32) + gate[None, :] * branch).astype(jnp.bfloat16)


def solution(mesh):
    sp, tp = mesh.shape["sp"], mesh.shape["tp"]

    def run(*args):
        heads = args[9].shape[1] // VALUE_DIM
        inner = Mesh(mesh.devices.reshape(sp // heads, heads, tp), ALL)
        in_specs = (
            P(ALL, None),
            P(SP, None),
            P("tp"),
            P("tp"),
            P("tp", SP),
            P(None, "tp"),
            P(None, "tp"),
            P(None, "tp"),
            P(None, "tp"),
            P(None, "tp"),
            P("tp"),
            P("tp"),
            P(),
            P("tp", None),
        )
        return jax.shard_map(
            body, mesh=inner, in_specs=in_specs, out_specs=P(ALL, None), check_vma=False
        )(*args)

    return run
```

```python
import functools
import math

import jax
import jax.numpy as jnp
from jax import lax
from jax.experimental import pallas as pl
from jax.experimental.pallas import tpu as pltpu
from jax.sharding import Mesh, PartitionSpec as P

HEAD_DIM = 64
VALUE_DIM = 128
GRID_W = 64
EPSILON = 1e-06
THETA = 10000.0
SP = ("g", "s")
ALL = ("g", "s", "tp")


def norm_rows(rows):
    values = rows.astype(jnp.float32)
    return values * lax.rsqrt(jnp.mean(values * values, axis=-1, keepdims=True) + EPSILON)


def shifts_over(array, axis, size):
    out = [array]
    for k in range(1, size):
        out.append(lax.ppermute(array, axis, [(i, (i + k) % size) for i in range(size)]))
    return out


def rope_tables(positions, extra):
    quarter = HEAD_DIM // 4
    reciprocal = THETA ** (-jnp.arange(quarter, dtype=jnp.float32) / quarter)
    row = (positions // GRID_W).astype(jnp.float32)[:, None] * reciprocal[None, :]
    col = (positions % GRID_W).astype(jnp.float32)[:, None] * reciprocal[None, :]
    angle = jnp.concatenate([row, row, col, col] * 2, -1)
    sign = jnp.where((jnp.arange(2 * HEAD_DIM) // quarter) % 2 == 0, -1.0, 1.0)
    cosine = jnp.cos(angle)
    sine = jnp.sin(angle) * sign[None, :]
    width = angle.shape[1]
    cosine = jnp.concatenate([cosine, jnp.ones((extra, width), jnp.float32)], 0)
    sine = jnp.concatenate([sine, jnp.zeros((extra, width), jnp.float32)], 0)
    return cosine, sine


def projection_kernel(parts, kinds, heads_dev, copies, first_row, base, lat, ctx, mod, cos, sin, *refs):
    weights, outs = refs[: parts * kinds], refs[parts * kinds :]
    rows = lat.shape[0]
    h_lat = norm_rows(lat[...]) * (1.0 + mod[2:3, :]) + mod[0:1, :]
    h_ctx = norm_rows(ctx[...]) * (1.0 + mod[3:4, :]) + mod[1:2, :]
    h = jnp.concatenate([h_lat, h_ctx], 0).astype(jnp.bfloat16)
    cosine, sine = cos[...], sin[...]
    lane = lax.broadcasted_iota(jnp.int32, cosine.shape, 1)
    quarter = HEAD_DIM // 4
    lower = (lane // quarter) % 2 == 0
    heads = parts * heads_dev
    for k in range(parts):
        products = [
            jnp.dot(h, w[...], preferred_element_type=jnp.float32)
            for w in weights[k * kinds : (k + 1) * kinds]
        ]
        for j in range(heads_dev):
            pair = jnp.concatenate(
                [p[:, j * HEAD_DIM : (j + 1) * HEAD_DIM] for p in products[:2]], 1
            )
            flipped = jnp.where(
                lower,
                pltpu.roll(pair, 2 * HEAD_DIM - quarter, 1),
                pltpu.roll(pair, quarter, 1),
            )
            turned = (pair * cosine + flipped * sine).astype(jnp.bfloat16)
            if kinds == 3:
                value = products[2][:, j * VALUE_DIM : (j + 1) * VALUE_DIM]
                value = value.astype(jnp.bfloat16)
            for copy in range(copies):
                slot = copy * heads + base[k] + j
                begin = 0
                for n, out in enumerate(outs):
                    size = first_row[n + 1] - first_row[n]
                    pieces = [(0, size, first_row[n])]
                    if n == 0 and out.shape[1] > size:
                        pieces.append((size, out.shape[1] - size, rows))
                    for at, length, source in pieces:
                        out[slot, at : at + length, : 2 * HEAD_DIM] = turned[
                            source : source + length
                        ]
                        if kinds == 3:
                            out[slot, at : at + length, 2 * HEAD_DIM :] = value[
                                source : source + length
                            ]


def project(base, latent, context, mod, cosine, sine, weights, heads_dev, copies, bounds, extra):
    parts, kinds = len(weights), len(weights[0])
    width = 2 * HEAD_DIM + (VALUE_DIM if kinds == 3 else 0)
    shapes = [
        jax.ShapeDtypeStruct(
            (copies * parts * heads_dev, bounds[n + 1] - bounds[n] + (extra if n == 0 else 0), width),
            jnp.bfloat16,
        )
        for n in range(len(bounds) - 1)
    ]
    vmem = pl.BlockSpec(memory_space=pltpu.VMEM)
    flat = [w for part in weights for w in part]
    return pl.pallas_call(
        functools.partial(projection_kernel, parts, kinds, heads_dev, copies, bounds),
        in_specs=[pl.BlockSpec(memory_space=pltpu.SMEM)] + [vmem] * (5 + len(flat)),
        out_specs=[vmem] * len(shapes),
        out_shape=shapes,
        compiler_params=pltpu.CompilerParams(vmem_limit_bytes=56 * 2**20),
        name="project_kv" if kinds == 3 else "project_q",
    )(base, latent, context, mod, cosine, sine, *flat)


def attention_kernel(first, last, rows, parts, scal, gain, q_ref, *refs):
    refs = list(refs)
    kvs, refs = refs[:parts], refs[parts:]
    extra = kvs[0].shape[1] - rows
    scratch = 4 if extra else 2
    scratches, refs = refs[-scratch:], refs[:-scratch]
    if not first:
        old, refs = refs[:4], refs[4:]
    out = refs
    width = 2 * HEAD_DIM

    @pl.when(pl.program_id(0) == 0)
    def _():
        for n, (begin, length) in enumerate(((0, rows), (rows, extra))[: scratch // 2]):
            keys, vals = scratches[2 * n], scratches[2 * n + 1]
            place = 0
            for kv in kvs:
                for i in range(kv.shape[0]):
                    keys[place : place + length, :] = kv[i, begin : begin + length, :width]
                    vals[place : place + length, :VALUE_DIM] = kv[i, begin : begin + length, width:]
                    place += length
            vals[:, VALUE_DIM:] = jnp.ones((vals.shape[0], VALUE_DIM), vals.dtype)

    q = q_ref[...]
    lane = lax.broadcasted_iota(jnp.int32, q.shape, 1)
    dims = (((1,), (1,)), ((), ()))
    results = []
    for m in range(2):
        query = jnp.where((lane < HEAD_DIM) == (m == 0), q, jnp.zeros_like(q))
        scores = []
        for n in range(scratch // 2):
            s = lax.dot_general(
                query, scratches[2 * n][...], dims, preferred_element_type=jnp.float32
            )
            scores.append(s + scal[0] if n else s)
        peak = functools.reduce(jnp.maximum, [jnp.max(s, axis=-1, keepdims=True) for s in scores])
        if not first:
            before = old[2 + m][...][:, :1]
            peak = jnp.maximum(peak, before)
        acc = 0.0
        for n, s in enumerate(scores):
            p = jnp.exp2(s - peak).astype(jnp.bfloat16)
            acc = acc + jnp.dot(p, scratches[2 * n + 1][...], preferred_element_type=jnp.float32)
        if not first:
            acc = acc + old[m][...] * jnp.exp2(before - peak)
        if last:
            results.append(acc[:, :VALUE_DIM] / acc[:, VALUE_DIM:])
        else:
            out[m][...] = acc
            out[2 + m][...] = jnp.broadcast_to(peak, (q.shape[0], 128))
    if last:
        mixed = results[0] - scal[1] * results[1]
        scale = lax.rsqrt(jnp.mean(mixed * mixed, axis=-1, keepdims=True) + EPSILON)
        out[0][...] = (mixed * scale * gain[...]).astype(out[0].dtype)


def attend(scal, gain, queries, kvs, rows, state, last):
    count = queries.shape[0]
    tile = math.gcd(count, 256)
    rows_spec = lambda width: pl.BlockSpec((tile, width), lambda i: (i, 0))
    state_shapes = [jax.ShapeDtypeStruct((count, w), jnp.float32) for w in (256, 256, 128, 128)]
    state_specs = [rows_spec(s.shape[1]) for s in state_shapes]
    first = state is None
    if last:
        shapes = jax.ShapeDtypeStruct((count, VALUE_DIM), jnp.bfloat16)
        specs = rows_spec(VALUE_DIM)
    else:
        shapes, specs = state_shapes, state_specs
    sources = kvs[0].shape[0] * len(kvs)
    scratch = []
    for length in (rows, kvs[0].shape[1] - rows):
        if length:
            scratch.append(pltpu.VMEM((sources * length, 2 * HEAD_DIM), jnp.bfloat16))
            scratch.append(pltpu.VMEM((sources * length, 2 * VALUE_DIM), jnp.bfloat16))
    return pl.pallas_call(
        functools.partial(attention_kernel, first, last, rows, len(kvs)),
        grid=(count // tile,),
        in_specs=[
            pl.BlockSpec(memory_space=pltpu.SMEM),
            pl.BlockSpec(gain.shape, lambda i: (0, 0)),
            rows_spec(2 * HEAD_DIM),
        ]
        + [pl.BlockSpec(kv.shape, lambda i: (0, 0, 0)) for kv in kvs]
        + ([] if first else state_specs),
        out_specs=specs,
        out_shape=shapes,
        scratch_shapes=scratch,
        compiler_params=pltpu.CompilerParams(
            dimension_semantics=("arbitrary",), vmem_limit_bytes=56 * 2**20
        ),
        name="attend_last" if last else "attend_first" if first else "attend_next",
    )(scal, gain, queries, *kvs, *([] if first else state))


def body(
    latent,
    context,
    condition,
    context_condition,
    modulation_weight,
    query_first,
    query_second,
    key_first,
    key_second,
    value_weight,
    lambda_head,
    context_score_boost,
    head_gain,
    output_weight,
):
    width = latent.shape[1]
    tp = lax.axis_size("tp")
    sp = lax.axis_size(SP)
    groups = lax.axis_size("g")
    t = lax.axis_index("tp")
    head = lax.axis_index("s")
    heads_dev = value_weight.shape[1] // VALUE_DIM
    heads = heads_dev * tp

    signal = jax.nn.silu(jnp.stack([condition, context_condition])).astype(jnp.bfloat16)
    partial_mod = jnp.dot(signal, modulation_weight, preferred_element_type=jnp.float32)
    columns = partial_mod.shape[1]
    message = jnp.concatenate([partial_mod.reshape(-1), lambda_head, context_score_boost])
    pad = -message.shape[0] % 128
    message = jnp.pad(message, (0, pad))
    received = lax.all_to_all(
        jnp.broadcast_to(message[None], (sp * tp, message.shape[0])), ALL, 0, 0
    ).reshape(sp, tp, -1)
    modulation = jnp.sum(received[:, :, : 2 * columns], axis=1).reshape(sp, 2, columns)
    modulation = jnp.transpose(modulation, (1, 0, 2)).reshape(2, sp * columns)
    lambdas = received[0, :, 2 * columns : 2 * columns + heads_dev].reshape(heads)
    boosts = received[0, :, 2 * columns + heads_dev : 2 * columns + 2 * heads_dev].reshape(heads)
    scal = jnp.stack([boosts[head] * math.log2(math.e), lambdas[head]])
    shift = modulation[:, :width]
    scale = modulation[:, width : 2 * width]
    gate = modulation[0, 2 * width :]

    packs = [
        shifts_over(w, "tp", tp)
        for w in (query_first, query_second, key_first, key_second, value_weight)
    ]
    out_weights = shifts_over(output_weight, "tp", tp)
    rows = latent.shape[0]
    rows_ctx = context.shape[0] // tp
    ctx_own = lax.dynamic_slice_in_dim(context, t * rows_ctx, rows_ctx, 0)
    mod = jnp.concatenate([shift, scale], 0)
    offset = (lax.axis_index(SP) * tp + t) * rows
    cosine, sine = rope_tables(offset + jnp.arange(rows, dtype=jnp.int32), rows_ctx)
    base = ((t - jnp.arange(tp, dtype=jnp.int32)) % tp) * heads_dev

    factor = HEAD_DIM ** (-0.5) * math.log2(math.e)
    (q_all,) = project(
        base, latent, ctx_own, mod, cosine * factor, sine * factor,
        [[packs[0][k], packs[1][k]] for k in range(tp)], heads_dev, 1, (0, rows), 0,
    )
    queries = lax.all_to_all(q_all, "s", 0, 0).reshape(heads * rows, 2 * HEAD_DIM)
    half = rows // 2
    sent = project(
        base, latent, ctx_own, mod, cosine, sine,
        [[packs[n][k] for n in (2, 3, 4)] for k in range(tp)],
        heads_dev, groups, (0, half, rows), rows_ctx,
    )
    gain = head_gain[None, :]
    state, order = None, queries
    arrived = []
    for chunk in sent:
        chunk, order = lax.optimization_barrier((chunk, order))
        order = lax.all_to_all(chunk, SP, 0, 0)
        arrived.append(order)
    for n, kv in enumerate(arrived):
        state = attend(scal, gain, queries, shifts_over(kv, "tp", tp), half, state, n == 1)
    heads_out = lax.all_to_all(state.reshape(heads, rows, VALUE_DIM), "s", 0, 0)

    grouped = heads_out.reshape(tp, heads_dev, rows, VALUE_DIM)
    branch = 0.0
    for k in range(tp):
        own = lax.dynamic_index_in_dim(grouped, (t - k) % tp, 0, keepdims=False)
        own = jnp.transpose(own, (1, 0, 2)).reshape(rows, heads_dev * VALUE_DIM)
        branch = branch + jnp.dot(own, out_weights[k], preferred_element_type=jnp.float32)
    return (latent.astype(jnp.float32) + gate[None, :] * branch).astype(jnp.bfloat16)


def solution(mesh):
    sp, tp = mesh.shape["sp"], mesh.shape["tp"]

    def run(*args):
        heads = args[9].shape[1] // VALUE_DIM
        inner = Mesh(mesh.devices.reshape(sp // heads, heads, tp), ALL)
        in_specs = (
            P(ALL, None),
            P(SP, None),
            P("tp"),
            P("tp"),
            P("tp", SP),
            P(None, "tp"),
            P(None, "tp"),
            P(None, "tp"),
            P(None, "tp"),
            P(None, "tp"),
            P("tp"),
            P("tp"),
            P(),
            P("tp", None),
        )
        return jax.shard_map(
            body, mesh=inner, in_specs=in_specs, out_specs=P(ALL, None), check_vma=False
        )(*args)

    return run
```

```python
import functools
import math

import jax
import jax.numpy as jnp
from jax import lax
from jax.experimental import pallas as pl
from jax.experimental.pallas import tpu as pltpu
from jax.sharding import Mesh, PartitionSpec as P

HEAD_DIM = 64
VALUE_DIM = 128
GRID_W = 64
EPSILON = 1e-06
THETA = 10000.0
SP = ("g", "s")
ALL = ("g", "s", "tp")


def norm_rows(rows):
    values = rows.astype(jnp.float32)
    return values * lax.rsqrt(jnp.mean(values * values, axis=-1, keepdims=True) + EPSILON)


def shifts_over(array, axis, size):
    out = [array]
    for k in range(1, size):
        out.append(lax.ppermute(array, axis, [(i, (i + k) % size) for i in range(size)]))
    return out


def rope_tables(positions, extra):
    quarter = HEAD_DIM // 4
    reciprocal = THETA ** (-jnp.arange(quarter, dtype=jnp.float32) / quarter)
    row = (positions // GRID_W).astype(jnp.float32)[:, None] * reciprocal[None, :]
    col = (positions % GRID_W).astype(jnp.float32)[:, None] * reciprocal[None, :]
    angle = jnp.concatenate([row, row, col, col] * 2, -1)
    sign = jnp.where((jnp.arange(2 * HEAD_DIM) // quarter) % 2 == 0, -1.0, 1.0)
    cosine = jnp.cos(angle)
    sine = jnp.sin(angle) * sign[None, :]
    width = angle.shape[1]
    cosine = jnp.concatenate([cosine, jnp.ones((extra, width), jnp.float32)], 0)
    sine = jnp.concatenate([sine, jnp.zeros((extra, width), jnp.float32)], 0)
    return cosine, sine


def projection_kernel(parts, kinds, heads_dev, copies, first_row, base, lat, ctx, mod, cos, sin, *refs):
    weights, outs = refs[: parts * kinds], refs[parts * kinds :]
    rows = lat.shape[0]
    h_lat = norm_rows(lat[...]) * (1.0 + mod[2:3, :]) + mod[0:1, :]
    h_ctx = norm_rows(ctx[...]) * (1.0 + mod[3:4, :]) + mod[1:2, :]
    h = jnp.concatenate([h_lat, h_ctx], 0).astype(jnp.bfloat16)
    cosine, sine = cos[...], sin[...]
    lane = lax.broadcasted_iota(jnp.int32, cosine.shape, 1)
    quarter = HEAD_DIM // 4
    lower = (lane // quarter) % 2 == 0
    heads = parts * heads_dev
    for k in range(parts):
        products = [
            jnp.dot(h, w[...], preferred_element_type=jnp.float32)
            for w in weights[k * kinds : (k + 1) * kinds]
        ]
        for j in range(heads_dev):
            pair = jnp.concatenate(
                [p[:, j * HEAD_DIM : (j + 1) * HEAD_DIM] for p in products[:2]], 1
            )
            flipped = jnp.where(
                lower,
                pltpu.roll(pair, 2 * HEAD_DIM - quarter, 1),
                pltpu.roll(pair, quarter, 1),
            )
            turned = (pair * cosine + flipped * sine).astype(jnp.bfloat16)
            if kinds == 3:
                value = products[2][:, j * VALUE_DIM : (j + 1) * VALUE_DIM]
                value = value.astype(jnp.bfloat16)
            for copy in range(copies):
                slot = copy * heads + base[k] + j
                begin = 0
                for n, out in enumerate(outs):
                    size = first_row[n + 1] - first_row[n]
                    pieces = [(0, size, first_row[n])]
                    if n == 0 and out.shape[1] > size:
                        pieces.append((size, out.shape[1] - size, rows))
                    for at, length, source in pieces:
                        out[slot, at : at + length, : 2 * HEAD_DIM] = turned[
                            source : source + length
                        ]
                        if kinds == 3:
                            out[slot, at : at + length, 2 * HEAD_DIM :] = value[
                                source : source + length
                            ]


def project(base, latent, context, mod, cosine, sine, weights, heads_dev, copies, bounds, extra):
    parts, kinds = len(weights), len(weights[0])
    width = 2 * HEAD_DIM + (VALUE_DIM if kinds == 3 else 0)
    shapes = [
        jax.ShapeDtypeStruct(
            (copies * parts * heads_dev, bounds[n + 1] - bounds[n] + (extra if n == 0 else 0), width),
            jnp.bfloat16,
        )
        for n in range(len(bounds) - 1)
    ]
    vmem = pl.BlockSpec(memory_space=pltpu.VMEM)
    flat = [w for part in weights for w in part]
    return pl.pallas_call(
        functools.partial(projection_kernel, parts, kinds, heads_dev, copies, bounds),
        in_specs=[pl.BlockSpec(memory_space=pltpu.SMEM)] + [vmem] * (5 + len(flat)),
        out_specs=[vmem] * len(shapes),
        out_shape=shapes,
        compiler_params=pltpu.CompilerParams(vmem_limit_bytes=56 * 2**20),
        name="project_kv" if kinds == 3 else "project_q",
    )(base, latent, context, mod, cosine, sine, *flat)


TILE = 512


def weights_of(scores, peak):
    return jnp.exp2(scores - peak).astype(jnp.bfloat16)


def attention_kernel(first, last, rows, parts, scal, gain, q_ref, *refs):
    refs = list(refs)
    kvs, refs = refs[:parts], refs[parts:]
    extra = kvs[0].shape[1] - rows
    scratch = 4 if extra else 2
    scratches, refs = refs[-scratch:], refs[:-scratch]
    if not first:
        old, refs = refs[:4], refs[4:]
    out = refs
    width = 2 * HEAD_DIM

    @pl.when(pl.program_id(0) == 0)
    def _():
        for n, (begin, length) in enumerate(((0, rows), (rows, extra))[: scratch // 2]):
            keys, vals = scratches[2 * n], scratches[2 * n + 1]
            place = 0
            for kv in kvs:
                for i in range(kv.shape[0]):
                    keys[place : place + length, :] = kv[i, begin : begin + length, :width]
                    vals[place : place + length, :VALUE_DIM] = kv[i, begin : begin + length, width:]
                    place += length
            vals[:, VALUE_DIM:] = jnp.ones((vals.shape[0], VALUE_DIM), vals.dtype)

    q = q_ref[...]
    lane = lax.broadcasted_iota(jnp.int32, q.shape, 1)
    dims = (((1,), (1,)), ((), ()))
    results = []
    for m in range(2):
        query = jnp.where((lane < HEAD_DIM) == (m == 0), q, jnp.zeros_like(q))
        scores = []
        for n in range(scratch // 2):
            s = lax.dot_general(
                query, scratches[2 * n][...], dims, preferred_element_type=jnp.float32
            )
            scores.append(s + scal[0] if n else s)
        peak = functools.reduce(jnp.maximum, [jnp.max(s, axis=-1, keepdims=True) for s in scores])
        if not first:
            before = old[2 + m][...][:, :1]
            peak = jnp.maximum(peak, before)
        acc = 0.0
        for n, s in enumerate(scores):
            p = weights_of(s, peak)
            acc = acc + jnp.dot(p, scratches[2 * n + 1][...], preferred_element_type=jnp.float32)
        if not first:
            acc = acc + old[m][...] * jnp.exp2(before - peak)
        if last:
            results.append(acc[:, :VALUE_DIM] / acc[:, VALUE_DIM:])
        else:
            out[m][...] = acc
            out[2 + m][...] = jnp.broadcast_to(peak, (q.shape[0], 128))
    if last:
        mixed = results[0] - scal[1] * results[1]
        scale = lax.rsqrt(jnp.mean(mixed * mixed, axis=-1, keepdims=True) + EPSILON)
        out[0][...] = (mixed * scale * gain[...]).astype(out[0].dtype)


def attend(scal, gain, queries, kvs, rows, state, last):
    count = queries.shape[0]
    tile = math.gcd(count, TILE)
    rows_spec = lambda width: pl.BlockSpec((tile, width), lambda i: (i, 0))
    state_shapes = [jax.ShapeDtypeStruct((count, w), jnp.float32) for w in (256, 256, 128, 128)]
    state_specs = [rows_spec(s.shape[1]) for s in state_shapes]
    first = state is None
    if last:
        shapes = jax.ShapeDtypeStruct((count, VALUE_DIM), jnp.bfloat16)
        specs = rows_spec(VALUE_DIM)
    else:
        shapes, specs = state_shapes, state_specs
    sources = kvs[0].shape[0] * len(kvs)
    scratch = []
    for length in (rows, kvs[0].shape[1] - rows):
        if length:
            scratch.append(pltpu.VMEM((sources * length, 2 * HEAD_DIM), jnp.bfloat16))
            scratch.append(pltpu.VMEM((sources * length, 2 * VALUE_DIM), jnp.bfloat16))
    return pl.pallas_call(
        functools.partial(attention_kernel, first, last, rows, len(kvs)),
        grid=(count // tile,),
        in_specs=[
            pl.BlockSpec(memory_space=pltpu.SMEM),
            pl.BlockSpec(gain.shape, lambda i: (0, 0)),
            rows_spec(2 * HEAD_DIM),
        ]
        + [pl.BlockSpec(kv.shape, lambda i: (0, 0, 0)) for kv in kvs]
        + ([] if first else state_specs),
        out_specs=specs,
        out_shape=shapes,
        scratch_shapes=scratch,
        compiler_params=pltpu.CompilerParams(
            dimension_semantics=("arbitrary",), vmem_limit_bytes=56 * 2**20
        ),
        name="attend_last" if last else "attend_first" if first else "attend_next",
    )(scal, gain, queries, *kvs, *([] if first else state))


def body(
    latent,
    context,
    condition,
    context_condition,
    modulation_weight,
    query_first,
    query_second,
    key_first,
    key_second,
    value_weight,
    lambda_head,
    context_score_boost,
    head_gain,
    output_weight,
):
    width = latent.shape[1]
    tp = lax.axis_size("tp")
    sp = lax.axis_size(SP)
    groups = lax.axis_size("g")
    t = lax.axis_index("tp")
    head = lax.axis_index("s")
    heads_dev = value_weight.shape[1] // VALUE_DIM
    heads = heads_dev * tp

    signal = jax.nn.silu(jnp.stack([condition, context_condition])).astype(jnp.bfloat16)
    partial_mod = jnp.dot(signal, modulation_weight, preferred_element_type=jnp.float32)
    columns = partial_mod.shape[1]
    message = jnp.concatenate([partial_mod.reshape(-1), lambda_head, context_score_boost])
    pad = -message.shape[0] % 128
    message = jnp.pad(message, (0, pad))
    received = lax.all_to_all(
        jnp.broadcast_to(message[None], (sp * tp, message.shape[0])), ALL, 0, 0
    ).reshape(sp, tp, -1)
    modulation = jnp.sum(received[:, :, : 2 * columns], axis=1).reshape(sp, 2, columns)
    modulation = jnp.transpose(modulation, (1, 0, 2)).reshape(2, sp * columns)
    lambdas = received[0, :, 2 * columns : 2 * columns + heads_dev].reshape(heads)
    boosts = received[0, :, 2 * columns + heads_dev : 2 * columns + 2 * heads_dev].reshape(heads)
    scal = jnp.stack([boosts[head] * math.log2(math.e), lambdas[head]])
    shift = modulation[:, :width]
    scale = modulation[:, width : 2 * width]
    gate = modulation[0, 2 * width :]

    packs = [
        shifts_over(w, "tp", tp)
        for w in (query_first, query_second, key_first, key_second, value_weight)
    ]
    out_weights = shifts_over(output_weight, "tp", tp)
    rows = latent.shape[0]
    rows_ctx = context.shape[0] // tp
    ctx_own = lax.dynamic_slice_in_dim(context, t * rows_ctx, rows_ctx, 0)
    mod = jnp.concatenate([shift, scale], 0)
    offset = (lax.axis_index(SP) * tp + t) * rows
    cosine, sine = rope_tables(offset + jnp.arange(rows, dtype=jnp.int32), rows_ctx)
    base = ((t - jnp.arange(tp, dtype=jnp.int32)) % tp) * heads_dev

    factor = HEAD_DIM ** (-0.5) * math.log2(math.e)
    (q_all,) = project(
        base, latent, ctx_own, mod, cosine * factor, sine * factor,
        [[packs[0][k], packs[1][k]] for k in range(tp)], heads_dev, 1, (0, rows), 0,
    )
    queries = lax.all_to_all(q_all, "s", 0, 0).reshape(heads * rows, 2 * HEAD_DIM)
    half = rows // 2
    sent = project(
        base, latent, ctx_own, mod, cosine, sine,
        [[packs[n][k] for n in (2, 3, 4)] for k in range(tp)],
        heads_dev, groups, (0, half, rows), rows_ctx,
    )
    gain = head_gain[None, :]
    state, order = None, queries
    arrived = []
    for chunk in sent:
        chunk, order = lax.optimization_barrier((chunk, order))
        order = lax.all_to_all(chunk, SP, 0, 0)
        arrived.append(order)
    for n, kv in enumerate(arrived):
        if n:
            kv, state = lax.optimization_barrier((kv, state))
        state = attend(scal, gain, queries, shifts_over(kv, "tp", tp), half, state, n == 1)
    heads_out = lax.all_to_all(state.reshape(heads, rows, VALUE_DIM), "s", 0, 0)

    grouped = heads_out.reshape(tp, heads_dev, rows, VALUE_DIM)
    branch = 0.0
    for k in range(tp):
        own = lax.dynamic_index_in_dim(grouped, (t - k) % tp, 0, keepdims=False)
        own = jnp.transpose(own, (1, 0, 2)).reshape(rows, heads_dev * VALUE_DIM)
        branch = branch + jnp.dot(own, out_weights[k], preferred_element_type=jnp.float32)
    return (latent.astype(jnp.float32) + gate[None, :] * branch).astype(jnp.bfloat16)


def solution(mesh):
    sp, tp = mesh.shape["sp"], mesh.shape["tp"]

    def run(*args):
        heads = args[9].shape[1] // VALUE_DIM
        inner = Mesh(mesh.devices.reshape(sp // heads, heads, tp), ALL)
        in_specs = (
            P(ALL, None),
            P(SP, None),
            P("tp"),
            P("tp"),
            P("tp", SP),
            P(None, "tp"),
            P(None, "tp"),
            P(None, "tp"),
            P(None, "tp"),
            P(None, "tp"),
            P("tp"),
            P("tp"),
            P(),
            P("tp", None),
        )
        return jax.shard_map(
            body, mesh=inner, in_specs=in_specs, out_specs=P(ALL, None), check_vma=False
        )(*args)

    return run
```
